32 devices in a mesh: ep: 8 (over z, y), tp: 4 (over x, core).
Axes of the slice: x: 2, y: 2, z: 4, core: 2. Of those that a mesh axis runs over, the one named last changes fastest.
Arguments:
- tokens: bfloat16 [2048, 2048], P('ep'), may hold values from -6 to 6
- cotangent: bfloat16 [2048, 2048], P('ep'), may hold values from -6 to 6
- gate_weights: bfloat16 [2048, 2], P('ep'), may hold values from 0.099609375 to 0.8984375
- routes: int32 [2048, 2], P('ep'), may hold values from 0 to 7, all different within a row; in each aligned block of 256 rows (0 to 255, 256 to 511, ...) at most 96 rows name the same one
- w_gate: bfloat16 [8, 2048, 3584], P('ep', None, 'tp'), may hold values from -0.125 to 0.125
- w_up: bfloat16 [8, 2048, 3584], P('ep', None, 'tp'), may hold values from -0.125 to 0.125
- w_down: bfloat16 [8, 3584, 2048], P('ep', 'tp'), may hold values from -0.09375 to 0.09375
Outputs:
- grad_tokens: bfloat16 [2048, 2048], P('ep', 'tp')
- grad_gates: float32 [2048, 2], P('ep')
- grad_w_gate: bfloat16 [8, 2048, 3584], P('ep', None, 'tp')
- grad_w_up: bfloat16 [8, 2048, 3584], P('ep', None, 'tp')
- grad_w_down: bfloat16 [8, 3584, 2048], P('ep', 'tp')
The draws below stay inside these ranges and needn't reach their ends.
Inputs may be any that keep to these rules, and one draw needn't show every extreme that they name: `routes`: each row names 2 different experts. Among the rows of one index of ep no expert is named by more than 96 rows, and this bound is reached in every draw.
All inputs are finite; a program needn't handle non-finite values.
Results may differ from the reference program's by a relative error of at most 0.012.
Values may be sent and summed in bfloat16 or wider, within the bound.
No kernel may reach another device: no remote copies, remote signals or barrier semaphores. Data moves between devices by JAX's collectives and lax.ppermute only.
A program may use at most 128 MiB of HBM per device.

```python
import math
import jax
import jax.numpy as jnp
import numpy as np
from jax import lax

D = 2048
FFE = 3584
TOPK = 2
TOK_DEV = 256
EXPERTS = 8
CAP = 96
TOKENS = 2048
N_EP = 8
N_TP = 4


def levels(key, extent, cuts, low, top_value):
    loudness, own = 1.0, jax.random.fold_in(key, 6)
    for position, shards_of in cuts:
        steps = jnp.exp(jax.random.uniform(jax.random.fold_in(own, position), (shards_of,), jnp.float32, low / len(cuts), top_value / len(cuts)))
        loudness = loudness * jnp.repeat(steps, extent[position] // shards_of).reshape([-1 if axis == position else 1 for axis in range(len(extent))])
    return loudness


def routed_block(own_key, own, number, rows, number_of, top, most, lean):
    order = jax.random.permutation(own_key, number_of)
    crowded, common = load_shares(number_of, rows * top, most, lean, True), load_shares(number_of, rows * top, most, lean, False)
    places = jnp.arange(number_of)

    def named(lengths, rotation):
        used = int((lengths > 0).sum())
        fixed = max(1, used // 4)
        passed = fixed + (places - fixed + rotation * (used - fixed)) % max(1, number_of - fixed)
        return jnp.zeros((number_of,), jnp.int32).at[order[jnp.where(places < fixed, places, passed)]].set(jnp.asarray(lengths, jnp.int32))

    lengths = jnp.where(number % 4 == 0, named(crowded, number // 4), named(common, number - number // 4 - 1))
    mixed = jax.random.permutation(jax.random.fold_in(own, 3), number_of)
    giver, receiver = mixed[0:number_of // 2 * 2:2], mixed[1:number_of // 2 * 2:2]
    room = jnp.minimum(lengths[giver] - 1, most - lengths[receiver]) // 2
    room = jnp.where((giver == order[0]) | (receiver == order[0]) | (lengths[receiver] == 0), 0, jnp.maximum(room, 0))
    passed = jax.random.randint(jax.random.fold_in(own, 4), (number_of // 2,), 0, 1 << 20) % (room + 1)
    lengths = lengths.at[giver].add(-passed).at[receiver].add(passed)
    items = jnp.searchsorted(jnp.cumsum(lengths), jnp.arange(rows * top), side="right").astype(jnp.int32)
    grid = items.reshape(top, rows).T
    grid = grid[jax.random.permutation(jax.random.fold_in(own, 1), rows)]
    rotation = jax.random.randint(jax.random.fold_in(own, 2), (rows, 1), 0, top)
    return jnp.take_along_axis(grid, (jnp.arange(top)[None, :] + rotation) % top, axis=1)


def load_shares(number_of, total, bound, slope, full):
    weights = [(1 << 20) // math.isqrt(grade ** slope) + 1 for grade in range(1, number_of + 1)]
    largest = bound if full else min(bound, max(-(-total // number_of), total * weights[0] // sum(weights)))
    least = 1 if total - largest >= number_of - 1 else 0
    holding, surplus = [largest] + [least] * (number_of - 1), total - largest - least * (number_of - 1)
    while surplus > 0:
        free = [i for i in range(1, number_of) if holding[i] < largest] or [i for i in range(1, number_of) if holding[i] < bound]
        pool, left = sum([weights[i] for i in free]), surplus
        for i in free:
            addition = min(bound - holding[i], max(1, left * weights[i] // pool), surplus)
            holding[i] = holding[i] + addition
            surplus = surplus - addition
    return np.array(holding)


def scatter_about(stream_key, extent, deviation, limit, cuts=(), kind=jnp.bfloat16):
    result = deviation * jax.random.normal(stream_key, extent, jnp.float32)
    if cuts:
        result = result * levels(stream_key, extent, cuts, -0.22, 0.18)
    return jnp.clip(result, -limit, limit).astype(kind)


def setup_inputs(seed: int = 0) -> dict:
    streams_of = jax.random.split(jax.random.key(seed), 8)
    tokens = scatter_about(streams_of[0], (TOKENS, D), 1.0, 6.0, ((0, 8),))
    cotangent = scatter_about(streams_of[1], (TOKENS, D), 1.0, 6.0, ((0, 8),))
    gate_weights = jnp.clip(0.099609375 + 0.7988281 * jax.random.uniform(streams_of[2], (TOKENS, TOPK), jnp.float32) ** levels(streams_of[2], (TOKENS, TOPK), ((0, 8),), -0.2, 0.2), 0.099609375, 0.8984375).astype(jnp.bfloat16)
    routes_keys = jax.random.split(jax.random.fold_in(streams_of[3], 1), TOKENS // TOK_DEV)
    routes_turns = jax.random.permutation(jax.random.fold_in(streams_of[3], 3), TOKENS // TOK_DEV)
    routes = jax.vmap(lambda own, number: routed_block(jax.random.fold_in(streams_of[3], 2), own, number, TOK_DEV, EXPERTS, TOPK, CAP, 2))(routes_keys, routes_turns).reshape((TOKENS, TOPK))
    w_gate = scatter_about(streams_of[4], (EXPERTS, D, FFE), D ** -0.5, 0.125, ((0, 8), (2, 4)))
    w_up = scatter_about(streams_of[5], (EXPERTS, D, FFE), D ** -0.5, 0.125, ((0, 8), (2, 4)))
    w_down = scatter_about(streams_of[6], (EXPERTS, FFE, D), FFE ** -0.5, 0.09375, ((0, 8), (1, 4)))
    return dict(tokens=tokens, cotangent=cotangent, gate_weights=gate_weights, routes=routes, w_gate=w_gate, w_up=w_up, w_down=w_down)


def reference(tokens, cotangent, gate_weights, routes, w_gate, w_up, w_down):
    pair_count = TOK_DEV * TOPK
    total = TOKENS * TOPK
    routed = routes.reshape(N_EP, pair_count)
    onehot = (routed[:, :, None] == jnp.arange(EXPERTS, dtype=jnp.int32)[None, None, :]).astype(jnp.int32)
    earlier = jnp.sum((jnp.cumsum(onehot, axis=1) - onehot) * onehot, axis=2)
    source = jnp.arange(N_EP, dtype=jnp.int32)[:, None]
    slot_of = routed * (N_EP * CAP) + source * CAP + earlier
    pair_of = source * pair_count + jnp.arange(pair_count, dtype=jnp.int32)[None, :]
    slot_pair = jnp.full((EXPERTS * N_EP * CAP,), total, jnp.int32)
    slot_pair = slot_pair.at[slot_of.reshape(-1)].set(pair_of.reshape(-1)).reshape(EXPERTS, N_EP * CAP)
    tok_pad = jnp.concatenate([tokens, jnp.zeros((1, D), jnp.bfloat16)], axis=0)
    cot_pad = jnp.concatenate([cotangent, jnp.zeros((1, D), jnp.bfloat16)], axis=0)
    gate_pad = jnp.concatenate([gate_weights.reshape(-1), jnp.zeros((1,), jnp.bfloat16)], axis=0)
    block_width = FFE // N_TP

    def expert_grads(packed):
        pair_ids, weight_gate, weight_up, weight_down = packed
        token_ids = jnp.where(pair_ids < total, pair_ids // TOPK, TOKENS).astype(jnp.int32)
        x_rows = tok_pad[token_ids]
        c_rows = cot_pad[token_ids]
        weights = gate_pad[pair_ids].astype(jnp.float32)
        gate_pre = jnp.dot(x_rows, weight_gate, preferred_element_type=jnp.float32)
        up_pre = jnp.dot(x_rows, weight_up, preferred_element_type=jnp.float32)
        logistic = jax.nn.sigmoid(gate_pre)
        activated = gate_pre * logistic
        hidden = (activated * up_pre).astype(jnp.bfloat16)
        back_hidden = jnp.dot(c_rows, weight_down.T, preferred_element_type=jnp.float32)
        pair_gate = jnp.sum(hidden.astype(jnp.float32) * back_hidden, axis=1)
        scaled = (weights[:, None] * c_rows.astype(jnp.float32)).astype(jnp.bfloat16)
        grad_down = jnp.dot(hidden.T, scaled, preferred_element_type=jnp.float32).astype(jnp.bfloat16)
        grad_hidden = weights[:, None] * back_hidden
        gate_grad = (grad_hidden * up_pre * logistic * (1.0 + gate_pre * (1.0 - logistic))).astype(jnp.bfloat16)
        up_grad = (grad_hidden * activated).astype(jnp.bfloat16)
        grad_gate_w = jnp.dot(x_rows.T, gate_grad, preferred_element_type=jnp.float32).astype(jnp.bfloat16)
        grad_up_w = jnp.dot(x_rows.T, up_grad, preferred_element_type=jnp.float32).astype(jnp.bfloat16)
        summed = jnp.zeros((x_rows.shape[0], D), jnp.float32)
        for block in range(N_TP):
            lower = block * block_width
            upper = lower + block_width
            part = jnp.dot(gate_grad[:, lower:upper], weight_gate[:, lower:upper].T, preferred_element_type=jnp.float32)
            part = part + jnp.dot(up_grad[:, lower:upper], weight_up[:, lower:upper].T, preferred_element_type=jnp.float32)
            summed = summed + part.astype(jnp.bfloat16).astype(jnp.float32)
        return grad_gate_w, grad_up_w, grad_down, summed.astype(jnp.bfloat16), pair_gate

    grad_w_gate, grad_w_up, grad_w_down, pair_rows, pair_gates = lax.map(
        expert_grads, (slot_pair, w_gate, w_up, w_down))
    flat_ids = slot_pair.reshape(-1)
    pair_grad = jnp.zeros((total, D), jnp.bfloat16).at[flat_ids].set(pair_rows.reshape(-1, D), mode="drop")
    grad_tokens = jnp.sum(pair_grad.reshape(TOKENS, TOPK, D).astype(jnp.float32), axis=1).astype(jnp.bfloat16)
    grad_gates = jnp.zeros((total,), jnp.float32).at[flat_ids].set(pair_gates.reshape(-1), mode="drop")
    return grad_tokens, grad_gates.reshape(TOKENS, TOPK), grad_w_gate, grad_w_up, grad_w_down
```

```python
import jax
import jax.numpy as jnp
from jax import lax
from jax.sharding import PartitionSpec as P

LAST = (((1,), (1,)), ((), ()))
FIRST = (((0,), (0,)), ((), ()))
F32 = jnp.float32
BF16 = jnp.bfloat16


def dot(a, b, dims):
    return lax.dot_general(a, b, dims, preferred_element_type=F32)


def rows16(count):
    return -(-count // 16) * 16


def flip(value, axis, mask):
    size = lax.axis_size(axis)
    return lax.ppermute(value, axis, [(i, i ^ mask) for i in range(size)])


def on_device(tokens, cotangent, gate_weights, routes, w_gate, w_up, w_down):
    tok_dev, width = tokens.shape
    top_k = routes.shape[1]
    groups = lax.axis_size("ep")
    narrow = lax.axis_size("tp")
    cap = 3 * top_k * tok_dev // (2 * groups)
    quarter = width // narrow
    me = lax.axis_index("ep")
    tp = lax.axis_index("tp")
    side, core = tp // 2, tp % 2
    wg, wu, wd = w_gate[0], w_up[0], w_down[0]

    wide = (1, 2, 3)
    first = (0,) + wide
    second = tuple(j for j in range(groups) if j not in first)

    rel = routes ^ me
    number = lax.broadcasted_iota(jnp.int32, (groups, tok_dev), 0)
    hits = [rel[:, k][None, :] == number for k in range(top_k)]
    mask = sum(h.astype(BF16) for h in hits)
    before = (
        lax.broadcasted_iota(jnp.int32, (tok_dev, tok_dev), 0)
        < lax.broadcasted_iota(jnp.int32, (tok_dev, tok_dev), 1)
    ).astype(BF16)
    place = jnp.dot(mask, before, preferred_element_type=F32).astype(jnp.int32)
    place = jnp.where(mask > 0, place, -1)
    select = (
        place[:, None, :] == lax.broadcasted_iota(jnp.int32, (groups, cap, tok_dev), 1)
    ).astype(BF16)
    weight_of = sum(
        h.astype(F32) * gate_weights[:, k].astype(F32)[None, :] for k, h in enumerate(hits)
    )
    sent_gate = jnp.sum(select.astype(F32) * weight_of[:, None, :], axis=2).astype(BF16)
    select_rows = select.reshape(groups * cap, tok_dev)

    def part(array, index):
        return lax.dynamic_slice_in_dim(array, index * quarter, quarter, 1)

    def picked(array, index):
        return dot(select_rows, part(array, index), (((1,), (0,)), ((), ()))).astype(BF16).reshape(
            groups, cap, quarter
        )

    near = (picked(tokens, tp), picked(cotangent, tp))
    far_tok, far_cot = part(tokens, tp ^ 2), part(cotangent, tp ^ 2)
    gate_rows = jnp.pad(sent_gate[:, None, :], ((0, 0), (0, 15), (0, quarter - cap)))

    def chosen(j, array):
        return dot(select[j], array, (((1,), (0,)), ((), ()))).astype(BF16)

    got = {}
    for j in wide + second:
        payload = jnp.concatenate([near[0][j], near[1][j], gate_rows[j]], axis=0)
        if j in wide:
            extra = jnp.concatenate([chosen(j, far_tok), chosen(j, far_cot)], axis=0)
            payload = jnp.concatenate([payload, extra], axis=0)
        got[j] = flip(payload, "ep", j)
    body = 2 * cap
    full = body + 16
    held = {}
    for j in wide:
        held[j] = (got[j][:body], got[j][full:])
    for j in second:
        held[j] = (got[j][:body], flip(got[j], "tp", 2)[:body])
    gates = {j: got[j][body, :cap].astype(F32) for j in wide + second}
    gates[0] = sent_gate[0].astype(F32)

    def assemble(members):
        mine_r = jnp.concatenate([held[j][0] for j in members], axis=0)
        mine_s = jnp.concatenate([held[j][1] for j in members], axis=0)
        mine = jnp.stack([mine_r, mine_s])
        theirs = flip(mine, "tp", 1)
        low = jnp.where(core == 0, mine, theirs)
        high = jnp.where(core == 0, theirs, mine)
        parts = [
            jnp.where(side == 0, low[0], low[1]),
            jnp.where(side == 0, high[0], high[1]),
            jnp.where(side == 0, low[1], low[0]),
            jnp.where(side == 0, high[1], high[0]),
        ]
        both = jnp.concatenate(parts, axis=1).reshape(len(members), 2, cap, width)
        count = len(members) * cap
        return both[:, 0].reshape(count, width), both[:, 1].reshape(count, width)

    def expert(x, c, g):
        gate_pre = jnp.dot(x, wg, preferred_element_type=F32)
        up_pre = jnp.dot(x, wu, preferred_element_type=F32)
        back = dot(c, wd, LAST)
        logistic = jax.nn.sigmoid(gate_pre)
        activated = gate_pre * logistic
        hidden = activated * up_pre
        gate_part = jnp.sum(hidden * back, axis=1)
        scaled = (g * hidden).astype(BF16)
        grad_hidden = g * back
        gate_grad = (grad_hidden * up_pre * logistic * (1.0 + gate_pre * (1.0 - logistic))).astype(
            BF16
        )
        up_grad = (grad_hidden * activated).astype(BF16)
        rows = dot(gate_grad, wg, LAST)
        rows = rows + dot(up_grad, wu, LAST)
        return rows, gate_part, scaled, gate_grad, up_grad

    def coded(values, count):
        top = lax.reduce_precision(values, 8, 7)
        low = values - top
        both = jnp.concatenate([top, low], axis=0).astype(BF16)
        return jnp.pad(both, ((0, rows16(2 * count) - 2 * count), (0, quarter - cap)))

    def decoded(block, count):
        return block[:count, :cap].astype(F32) + block[count : 2 * count, :cap].astype(F32)

    def reduced(rows, gate_part, count):
        rows = rows.astype(BF16)
        total = rows.shape[0]
        q = [rows[:, i * quarter : (i + 1) * quarter] for i in range(narrow)]
        low, high = (q[0], q[2]), (q[1], q[3])
        keep = [jnp.where(core == 0, a, b) for a, b in zip(low, high)]
        send = [jnp.where(core == 0, b, a) for a, b in zip(low, high)]
        sums = gate_part.reshape(count, cap)
        came = flip(jnp.concatenate(send + [coded(sums, count)], axis=0), "tp", 1)
        sums = sums + decoded(came[2 * total :], count)
        a = keep[0].astype(F32) + came[:total].astype(F32)
        b = keep[1].astype(F32) + came[total : 2 * total].astype(F32)
        stay = jnp.where(side == 0, a, b)
        leave = jnp.where(side == 0, b, a).astype(BF16)
        came = flip(jnp.concatenate([leave, coded(sums, count)], axis=0), "tp", 2)
        sums = sums + decoded(came[total:], count)
        done = (stay + came[:total].astype(F32)).astype(BF16)
        return done.reshape(count, cap, quarter), sums

    rows_back, gates_back = {}, {}
    xs, cs, hs, gg, ug = [], [], [], [], []
    for members in (first, second):
        x, c = None, None
        others = tuple(j for j in members if j != 0)
        x, c = assemble(others)
        if 0 in members:
            x = jnp.concatenate([chosen(0, tokens), x], axis=0)
            c = jnp.concatenate([chosen(0, cotangent), c], axis=0)
        g = jnp.concatenate([gates[j] for j in members])[:, None]
        rows, gate_part, scaled, gate_grad, up_grad = expert(x, c, g)
        xs.append(x)
        cs.append(c)
        hs.append(scaled)
        gg.append(gate_grad)
        ug.append(up_grad)
        done, sums = reduced(rows, gate_part, len(members))
        for i, j in enumerate(members):
            if j == 0:
                rows_back[j], gates_back[j] = done[i], sums[i]
                continue
            came = flip(jnp.concatenate([done[i], coded(sums[i : i + 1], 1)], axis=0), "ep", j)
            rows_back[j] = came[:cap]
            gates_back[j] = decoded(came[cap:], 1)[0]

    x_all, c_all = jnp.concatenate(xs), jnp.concatenate(cs)
    grad_gate_w = dot(x_all, jnp.concatenate(gg), FIRST).astype(BF16)
    grad_up_w = dot(x_all, jnp.concatenate(ug), FIRST).astype(BF16)
    grad_down = dot(jnp.concatenate(hs), c_all, FIRST).astype(BF16)

    back = jnp.concatenate([rows_back[j] for j in range(groups)], axis=0)
    grad_tokens = dot(select_rows, back, FIRST).astype(BF16)
    back_gate = jnp.stack([gates_back[j] for j in range(groups)])
    at_token = jnp.sum(select.astype(F32) * back_gate[:, :, None], axis=1)
    grad_gates = jnp.stack([jnp.sum(h.astype(F32) * at_token, axis=0) for h in hits], axis=1)
    return (grad_tokens, grad_gates, grad_gate_w[None], grad_up_w[None], grad_down[None])


def solution(mesh):
    tok = P("ep", None)
    in_specs = (tok, tok, tok, tok, P("ep", None, "tp"), P("ep", None, "tp"), P("ep", "tp", None))
    out_specs = (P("ep", "tp"), tok, P("ep", None, "tp"), P("ep", None, "tp"), P("ep", "tp", None))


    return jax.shard_map(
        on_device, mesh=mesh, in_specs=in_specs, out_specs=out_specs, check_vma=False
    )
```
